128 devices in a mesh: fs: 16 (over z, y), tp: 8 (over x, core).
Axes of the slice: x: 4, y: 4, z: 4, core: 2. Of those that a mesh axis runs over, the one named last changes fastest.
Arguments:
- tokens: bfloat16 [24576, 2048], P(('fs', 'tp')), may hold values from -60 to 60
- norm_gain: float32 [2048], P('fs'), may hold values from 0.1 to 1.9
- gate_weight: float32 [2048, 5632], P('fs', 'tp'), may hold values from -0.125 to 0.125
- up_weight: float32 [2048, 5632], P('fs', 'tp'), may hold values from -0.125 to 0.125
- down_weight: float32 [2048, 5632], P('fs', 'tp'), may hold values from -0.078125 to 0.078125
Outputs:
- mixed_rows: bfloat16 [24576, 2048], P(('fs', 'tp'))
- gate_out: bfloat16 [2048, 5632], P(None, 'tp')
- up_out: bfloat16 [2048, 5632], P(None, 'tp')
- down_out: bfloat16 [2048, 5632], P(None, 'tp')
The draws below stay inside these ranges and needn't reach their ends.
All inputs are finite; a program needn't handle non-finite values.
Results may differ from the reference program's by a relative error of at most 0.014.
Values may be sent and summed in bfloat16 or wider, within the bound.
No kernel may reach another device: no remote copies, remote signals or barrier semaphores. Data moves between devices by JAX's collectives and lax.ppermute only.
A program may use at most 128 MiB of HBM per device.

```python
import math
import jax
import jax.numpy as jnp
from jax import lax

D = 2048
FF = 5632
TOKENS = 24576
N_TP = 8


def draw_tokens(key, part):
    key_base = jax.random.fold_in(key, 11)
    key_scale = jax.random.fold_in(key, 12)
    standard = jnp.clip(jax.random.normal(key_base, (TOKENS, D), jnp.float32), -6.0, 6.0)
    scales = jnp.exp(jax.random.uniform(key_scale, (TOKENS, 1), jnp.float32, math.log(0.3), math.log(3.0)))
    return (standard * scales).astype(jnp.bfloat16)


def levels(stream_key, dims, shards, low, largest):
    level = 1.0
    for axis_at, shards_of in shards:
        draws = jax.random.uniform(jax.random.fold_in(jax.random.fold_in(stream_key, 6), axis_at), (shards_of,), jnp.float32, low / len(shards), largest / len(shards))
        level = level * jnp.repeat(jnp.exp(draws), dims[axis_at] // shards_of).reshape((-1,) + (1,) * (len(dims) - 1 - axis_at))
    return level


def bell_draw(key, dims, scale, bound, pieces=(), kind=jnp.bfloat16):
    entries = scale * jax.random.normal(key, dims, jnp.float32)
    if pieces:
        entries = entries * levels(key, dims, pieces, -0.22, 0.18)
    return jnp.clip(entries, -bound, bound).astype(kind)


def setup_inputs(seed: int = 0) -> dict:
    splits = jax.random.split(jax.random.key(seed), 6)
    return {
        "tokens": draw_tokens(jax.random.fold_in(splits[5], 71), 0),
        "norm_gain": jnp.clip(1.0 + 0.18 * jax.random.normal(splits[1], (D,), jnp.float32), 0.1, 1.9),
        "gate_weight": bell_draw(splits[2], (D, FF), D ** -0.5, 0.125, ((0, 16), (1, 8)), jnp.float32),
        "up_weight": bell_draw(splits[3], (D, FF), D ** -0.5, 0.125, ((0, 16), (1, 8)), jnp.float32),
        "down_weight": bell_draw(splits[4], (D, FF), FF ** -0.5, 0.078125, ((0, 16), (1, 8)), jnp.float32),
    }


def reference(tokens, norm_gain, gate_weight, up_weight, down_weight):
    row_gain = norm_gain[:, None]
    gate_out = (gate_weight * row_gain).astype(jnp.bfloat16)
    up_out = (up_weight * row_gain).astype(jnp.bfloat16)
    down_out = down_weight.astype(jnp.bfloat16)
    widened = tokens.astype(jnp.float32)
    normed = (widened * lax.rsqrt(lax.optimization_barrier(jnp.mean(widened * widened, axis=1, keepdims=True)) + 1e-06)).astype(jnp.bfloat16)
    gate_pre = jnp.dot(normed, gate_out, preferred_element_type=jnp.float32)
    up_pre = jnp.dot(normed, up_out, preferred_element_type=jnp.float32)
    hidden = (jax.nn.silu(gate_pre) * up_pre).astype(jnp.bfloat16)
    block_width = FF // N_TP
    running = jnp.zeros((tokens.shape[0], D), jnp.float32)
    for block in range(N_TP):
        lower = block * block_width
        partial_value = lax.dot_general(hidden[:, lower:lower + block_width], down_out[:, lower:lower + block_width], (((1,), (1,)), ((), ())), preferred_element_type=jnp.float32)
        partial_value = lax.optimization_barrier(partial_value.astype(jnp.bfloat16)).astype(jnp.float32)
        running = running + partial_value
    return (running.astype(jnp.bfloat16), gate_out, up_out, down_out)
```

```python
import functools

import jax
import jax.numpy as jnp
from jax import lax
from jax.experimental import pallas as pl
from jax.experimental.pallas import tpu as pltpu
from jax.sharding import PartitionSpec as P


ANY = pl.BlockSpec(memory_space=pl.ANY)
OFF = (0, -1, 1, 2)
F32, BF16 = jnp.float32, jnp.bfloat16


def moves(kind):
    axis, by = kind[0], int(kind[1:])
    if axis in "zy":
        step = lambda z, y: ((z + by) % 4, y) if axis == "z" else (z, (y + by) % 4)
        return "fs", [(z * 4 + y, step(z, y)[0] * 4 + step(z, y)[1]) for z in range(4) for y in range(4)]
    step = lambda x, c: ((x + by) % 4, c) if axis == "x" else (x, 1 - c)
    return "tp", [(x * 2 + c, step(x, c)[0] * 2 + step(x, c)[1]) for x in range(4) for c in range(2)]


def send(a, kind):
    axis, pairs = moves(kind)
    return lax.ppermute(a, axis, pairs)


def spots():
    at = lax.axis_index("fs")
    turned = lambda v: [lax.rem(v + o + 4, 4) for o in OFF]
    return turned(at // 4), turned(lax.rem(at, 4))


def lanes(block, width=128):
    return pl.ds(pl.multiple_of(block * width, width), width)


def copy(src, dst, sem):
    c = pltpu.make_async_copy(src, dst, sem)
    c.start()
    return c


def gu_body(rels, sides, first, last, rows, *refs):
    refs = list(refs)
    take = lambda n: [refs.pop(0) for _ in range(n)]
    toks = take(4)
    pieces = [[take(4) for _ in rels] for _ in range(sides)]
    accs = None if first else [take(2) for _ in range(sides)]
    outs = [take(1 if last else 2) for _ in range(sides)]
    tok_v, w_v, acc_v, sem_t, sem_w, sem_a, sem_o = take(7)
    h_v = take(1)[0] if last else None
    zs, ys = spots()
    tc = [copy(t, tok_v.at[pl.ds(i * 192, 192)], sem_t.at[i]) for i, t in enumerate(toks)]
    wc, ac, oc = {}, {}, []
    for s in range(sides):
        for m in range(2):
            wc[s, m] = [
                copy(
                    pieces[s][q][m * 2 + half].at[k, pl.ds(0, 704)],
                    w_v.at[s, m, :, lanes(q * 4 + (zs if m else ys)[half * 2 + k])],
                    sem_w.at[s, m, q * 4 + half * 2 + k],
                )
                for q in range(len(rels))
                for half in range(2)
                for k in range(2)
            ]
            if not first:
                ac[s, m] = copy(accs[s][m], acc_v.at[s, m], sem_a.at[s, m])
    for c in tc:
        c.wait()
    for s in range(sides):
        for m in range(2):
            for c in wc[s, m]:
                c.wait()
            if not first:
                ac[s, m].wait()
            for r0 in range(0, 768, rows):
                rs = pl.ds(r0, rows)
                cols = []
                for r in rels:
                    if m:
                        cols += [tok_v[rs, lanes(z * 4 + ys[r])] for z in range(4)]
                    else:
                        cols.append(tok_v[rs, lanes(zs[r], 512)])
                new = lax.dot_general(
                    jnp.concatenate(cols, axis=1), w_v[s, m], (((1,), (1,)), ((), ())), preferred_element_type=F32
                )
                if not first:
                    new = new + acc_v[s, m, rs]
                if last and m:
                    g = acc_v[s, 0, rs]
                    h_v[s, rs, pl.ds(0, 704)] = (g / (1.0 + jnp.exp(-g)) * new).astype(BF16)
                    h_v[s, rs, pl.ds(704, 64)] = jnp.zeros((rows, 64), BF16)
                else:
                    acc_v[s, m, rs] = new
            if not last:
                oc.append(copy(acc_v.at[s, m], outs[s][m], sem_o.at[s, m]))
        if last:
            oc.append(copy(h_v.at[s], outs[s][0], sem_o.at[s, 0]))
    for c in oc:
        c.wait()


def gu(tokens, pieces, rels, accs=None, last=False, rows=384):
    sides, n = len(pieces), len(rels)
    flat = list(tokens)
    for s in pieces:
        for r in rels:
            flat += [*s[0][r], *s[1][r]]
    for a in accs or []:
        flat += a
    if last:
        outs = [jax.ShapeDtypeStruct((768, 768), BF16)] * sides
    else:
        outs = [jax.ShapeDtypeStruct((768, 704), F32)] * (2 * sides)
    scratch = [
        pltpu.VMEM((768, 2048), BF16),
        pltpu.VMEM((sides, 2, 704, 512 * n), BF16),
        pltpu.VMEM((sides, 2, 768, 704), F32),
        pltpu.SemaphoreType.DMA((4,)),
        pltpu.SemaphoreType.DMA((sides, 2, 4 * n)),
        pltpu.SemaphoreType.DMA((sides, 2)),
        pltpu.SemaphoreType.DMA((sides, 2)),
    ]
    if last:
        scratch.append(pltpu.VMEM((sides, 768, 768), BF16))
    flops = sides * 4 * 768 * 704 * 512 * n
    got = pl.pallas_call(
        functools.partial(gu_body, rels, sides, accs is None, last, rows),
        out_shape=outs,
        in_specs=[ANY] * len(flat),
        out_specs=[ANY] * len(outs),
        scratch_shapes=scratch,
        compiler_params=pltpu.CompilerParams(vmem_limit_bytes=60 * 1024 * 1024),
        cost_estimate=pl.CostEstimate(flops=flops, bytes_accessed=flops // 400, transcendentals=0),
        name=f"gu{len(rels)}{sides}{int(last)}",
    )(*flat)
    return list(got) if last else [list(got[2 * s : 2 * s + 2]) for s in range(sides)]


def down_body(rels, rows, *refs):
    refs = list(refs)
    take = lambda n: [refs.pop(0) for _ in range(n)]
    hid = take(2)
    pieces = [[(take(2), take(4)) for _ in rels] for _ in range(2)]
    outs = take(4)
    h_v, w_v, p_v, sem_h, sem_w, sem_o = take(6)
    _, ys = spots()
    hc = [copy(h, h_v.at[:, pl.ds(768 * s, 768)], sem_h.at[s]) for s, h in enumerate(hid)]
    wc = []
    for q, r in enumerate(rels):
        for s in range(2):
            top, bottom = pieces[s][q]
            base = s * 768
            for j in range(4):
                at = lanes(q * 4 + ys[j])
                wc.append(copy(top[j // 2].at[j % 2, pl.ds(704, 352)], w_v.at[pl.ds(base, 352), at], sem_w.at[q, s, 0, j]))
                wc.append(copy(bottom[j].at[r % 2, pl.ds(704, 352)], w_v.at[pl.ds(base + 352, 352), at], sem_w.at[q, s, 1, j]))
    for s in range(2):
        w_v[pl.ds(s * 768 + 704, 64), :] = jnp.zeros((64, 512 * len(rels)), BF16)
    for c in hc + wc:
        c.wait()
    oc = []
    for i in range(4):
        for r0 in range(0, 192, rows):
            p_v[i, pl.ds(r0, rows)] = jnp.dot(
                h_v[pl.ds(i * 192 + r0, rows)], w_v[...], preferred_element_type=F32
            ).astype(BF16)
        oc.append(copy(p_v.at[i], outs[i], sem_o.at[i]))
    for c in oc:
        c.wait()


def down(hidden, pieces, rels, rows=192):
    n = len(rels)
    flat = list(hidden)
    for top, bottom in pieces:
        for r in rels:
            flat += [*top[r], *(b[r // 2] for b in bottom)]
    flops = 2 * 768 * 1408 * 512 * n
    return pl.pallas_call(
        functools.partial(down_body, rels, rows),
        out_shape=[jax.ShapeDtypeStruct((192, 512 * n), BF16)] * 4,
        in_specs=[ANY] * len(flat),
        out_specs=[ANY] * 4,
        scratch_shapes=[
            pltpu.VMEM((768, 1536), BF16),
            pltpu.VMEM((1536, 512 * n), BF16),
            pltpu.VMEM((4, 192, 512 * n), BF16),
            pltpu.SemaphoreType.DMA((2,)),
            pltpu.SemaphoreType.DMA((n, 2, 2, 4)),
            pltpu.SemaphoreType.DMA((4,)),
        ],
        compiler_params=pltpu.CompilerParams(vmem_limit_bytes=60 * 1024 * 1024),
        cost_estimate=pl.CostEstimate(flops=flops, bytes_accessed=flops // 400, transcendentals=0),
        name=f"down{n}",
    )(*flat)


def whole_body(*refs):
    a, b = refs[:8], refs[8:16]
    outs, (w_v, sem_w, sem_o) = refs[16:19], refs[19:]
    zs, ys = spots()
    got = [[], [], []]
    for q in range(4):
        for j in range(4):
            half, k = j // 2, j % 2
            at, bt = lanes(zs[q] * 4 + ys[j]), lanes(zs[j] * 4 + ys[q])
            ra, rb = a[q * 2 + half].at[k], b[q * 2 + half].at[k]
            got[0].append(copy(ra.at[pl.ds(0, 704)], w_v.at[0, :, at], sem_w.at[0, q, j]))
            got[1].append(copy(rb.at[pl.ds(0, 704)], w_v.at[1, :, bt], sem_w.at[1, q, j]))
            got[2].append(copy(ra.at[pl.ds(704, 352)], w_v.at[2, pl.ds(0, 352), at], sem_w.at[2, q, j]))
            got[2].append(copy(rb.at[pl.ds(704, 352)], w_v.at[2, pl.ds(352, 352), bt], sem_w.at[3, q, j]))
    oc = []
    for m in range(3):
        for c in got[m]:
            c.wait()
        oc.append(copy(w_v.at[m], outs[m], sem_o.at[m]))
    for c in oc:
        c.wait()


def whole(a, b):
    flat = [v for pair in (*a, *b) for v in pair]
    return pl.pallas_call(
        whole_body,
        out_shape=[jax.ShapeDtypeStruct((704, 2048), BF16)] * 3,
        in_specs=[ANY] * 16,
        out_specs=[ANY] * 3,
        scratch_shapes=[
            pltpu.VMEM((3, 704, 2048), BF16),
            pltpu.SemaphoreType.DMA((4, 4, 4)),
            pltpu.SemaphoreType.DMA((3,)),
        ],
        compiler_params=pltpu.CompilerParams(vmem_limit_bytes=60 * 1024 * 1024),
        cost_estimate=pl.CostEstimate(flops=2 * 10**9, bytes_accessed=17 * 10**6, transcendentals=0),
        name="whole",
    )(*flat)


def mix_body(chunks, *refs):
    out = refs[-1]
    zs, _ = spots()
    for c, rels in enumerate(chunks):
        total = sum(refs[c * 4 + i][...].astype(F32) for i in range(4)).astype(BF16)
        for q, r in enumerate(rels):
            out[:, lanes(zs[r], 512)] = total[:, q * 512 : (q + 1) * 512]


def mix(parts, chunks):
    flat = [v for p in parts for v in p]
    return pl.pallas_call(
        functools.partial(mix_body, chunks),
        out_shape=jax.ShapeDtypeStruct((192, 2048), BF16),
        compiler_params=pltpu.CompilerParams(vmem_limit_bytes=60 * 1024 * 1024),
        cost_estimate=pl.CostEstimate(flops=10**8, bytes_accessed=4 * 10**6, transcendentals=0),
        name="mix",
    )(*flat)


def ring_row(a, axis):
    before, after, far = send(a, axis + "1"), send(a, axis + "-1"), send(a, axis + "2")
    return jnp.stack([a, before]), jnp.stack([after, far])


def ring_rows(lo, hi, axis):
    up, dn = axis + "1", axis + "-1"
    lo1, hi2 = send(lo, up), send(hi, dn)
    hi1, lo2 = send(hi, up), send(lo, dn)
    return [(lo, hi), (lo1, hi1), (lo2, hi2), (send(lo1, up), send(hi2, dn))]


def shards(tokens, norm_gain, gate_weight, up_weight, down_weight):
    gain = norm_gain[None, :]
    gate_t = (gate_weight.T * gain).astype(BF16)
    up_t = (up_weight.T * gain).astype(BF16)
    down_t = down_weight.T.astype(BF16)
    wide = tokens.astype(F32)
    normed = (wide * lax.rsqrt(jnp.mean(wide * wide, axis=1, keepdims=True) + 1e-06)).astype(BF16)

    a = ring_rows(*ring_row(jnp.concatenate([gate_t, down_t[:352]]), "y"), "z")
    b = ring_rows(*ring_row(jnp.concatenate([up_t, down_t[352:]]), "z"), "y")
    rows = [normed, send(normed, "x1"), send(normed, "x-1"), send(normed, "x2")]
    other = lambda side: [tuple(send(v, "c1") for v in pair) for pair in side]
    own, partner = (a, b), (other(a), other(b))

    acc = gu(rows, (own, partner), (0,))
    acc = gu(rows, (own, partner), (1, 2), acc)
    hidden = gu(rows, (own,), (3,), acc[:1], True) + gu(rows, (partner,), (3,), acc[1:], True)
    chunks = ((0, 1), (2, 3))
    parts = []
    for rels in chunks:
        mine, before, after, far = down(hidden, (own, partner), rels)
        parts.append([mine, send(before, "x-1"), send(after, "x1"), send(far, "x2")])
    gate_whole, up_whole, down_whole = whole(a, b)
    return mix(parts, chunks), gate_whole.T, up_whole.T, down_whole.T


def solution(mesh):
    in_specs = (P(("fs", "tp"), None), P("fs"), P("fs", "tp"), P("fs", "tp"), P("fs", "tp"))
    out_specs = (P(("fs", "tp"), None), P(None, "tp"), P(None, "tp"), P(None, "tp"))
    return jax.shard_map(shards, mesh=mesh, in_specs=in_specs, out_specs=out_specs, check_vma=False)
```

```python
import functools

import jax
import jax.numpy as jnp
from jax import lax
from jax.experimental import pallas as pl
from jax.experimental.pallas import tpu as pltpu
from jax.sharding import PartitionSpec as P


ANY = pl.BlockSpec(memory_space=pl.ANY)
OFF = (0, -1, 1, 2)
F32, BF16 = jnp.float32, jnp.bfloat16


def pairs(step):
    out = []
    for z in range(4):
        for y in range(4):
            for x in range(4):
                for c in range(2):
                    a, b, d = (v % 4 for v in step(z, y, x, c))
                    out.append((((z * 4 + y) * 4 + x) * 2 + c, ((a * 4 + b) * 4 + d) * 2 + c))
    return out


def send(a, ring, by):
    if ring == "x":
        move = lambda z, y, x, c: (z, y, x + by)
    else:
        move = lambda z, y, x, c: (z + by, y, x) if (ring == "first") == (c == 1) else (z, y + by, x)
    return lax.ppermute(a, ("fs", "tp"), pairs(move))


def swap(a):
    return lax.ppermute(a, "tp", [(i, i ^ 1) for i in range(8)])


def core():
    return lax.rem(lax.axis_index("tp"), 2)


def spots(flip):
    at = lax.axis_index("fs")
    turned = lambda v: [lax.rem(v + o + 4, 4) for o in OFF]
    z, y = turned(at // 4), turned(lax.rem(at, 4))
    here = [jnp.where(flip == 0, 4 * u, v) for u, v in zip(z, y)]
    there = [jnp.where(flip == 0, v, 4 * u) for u, v in zip(z, y)]
    return lambda q, j: here[q] + there[j]


def lanes(block):
    return pl.ds(pl.multiple_of(block * 128, 128), 128)


def copy(src, dst, sem):
    c = pltpu.make_async_copy(src, dst, sem)
    c.start()
    return c


PLACE = (0, 192, 384, 576, 672)
FULL = pltpu.CompilerParams(vmem_limit_bytes=60 * 1024 * 1024)


def call(body, out_shape, operands, scratch, flops):
    return pl.pallas_call(
        body,
        out_shape=out_shape,
        in_specs=[ANY] * len(operands),
        out_specs=jax.tree.map(lambda _: ANY, out_shape),
        scratch_shapes=scratch,
        compiler_params=FULL,
        cost_estimate=pl.CostEstimate(flops=flops, bytes_accessed=flops // 400, transcendentals=0),
    )(*operands)


def product(x, w):
    return lax.dot_general(x, w, (((1,), (1,)), ((), ())), preferred_element_type=F32)


def gu_body(rels, theirs, first, rows, *refs):
    refs = list(refs)
    take = lambda n: [refs.pop(0) for _ in range(n)]
    toks = take(5)
    pieces = [take(2) for _ in rels]
    acc = None if first else take(1)[0]
    out, tok_v, w_v, acc_v, sem_t, sem_w, sem_a, sem_o = take(8)
    c = core()
    at = spots(1 - c if theirs else c)
    wc, ac, oc = [], [], []
    for s in range(2):
        wc.append(
            [
                copy(
                    pieces[q][j // 2].at[j % 2, s, pl.ds(0, 704)],
                    w_v.at[s, :, pl.ds((q * 4 + j) * 128, 128)],
                    sem_w.at[s, q * 4 + j],
                )
                for q in range(len(rels))
                for j in range(4)
            ]
        )
        if s == 0:
            tc = [
                copy(
                    toks[i].at[:, lanes(at(r, j))],
                    tok_v.at[pl.ds(PLACE[i], 192 if i < 3 else 96), pl.ds((q * 4 + j) * 128, 128)],
                    sem_t.at[i, q * 4 + j],
                )
                for i in range(5)
                for q, r in enumerate(rels)
                for j in range(4)
            ]
        if not first:
            ac.append(copy(acc.at[s], acc_v.at[s], sem_a.at[s]))
    for s in range(2):
        for v in wc[s] + (tc if s == 0 else []):
            v.wait()
        if not first:
            ac[s].wait()
        for r0 in range(0, 768, rows):
            rs = pl.ds(r0, rows)
            new = product(tok_v[rs], w_v[s])
            acc_v[s, rs] = new if first else new + acc_v[s, rs]
        oc.append(copy(acc_v.at[s], out.at[s], sem_o.at[s]))
    for v in oc:
        v.wait()


def gu(tokens, half, rels, theirs, acc=None, rows=384):
    n = len(rels)
    operands = list(tokens) + [v for r in rels for v in half[r]] + ([] if acc is None else [acc])
    scratch = [
        pltpu.VMEM((768, 512 * n), BF16),
        pltpu.VMEM((2, 704, 512 * n), BF16),
        pltpu.VMEM((2, 768, 704), F32),
        pltpu.SemaphoreType.DMA((5, 4 * n)),
        pltpu.SemaphoreType.DMA((2, 4 * n)),
        pltpu.SemaphoreType.DMA((2,)),
        pltpu.SemaphoreType.DMA((2,)),
    ]
    body = functools.partial(gu_body, rels, theirs, acc is None, rows)
    return call(body, jax.ShapeDtypeStruct((2, 768, 704), F32), operands, scratch, 4 * 768 * 704 * 512 * n)


def fin_body(which, *refs):
    refs = list(refs)
    take = lambda n: [refs.pop(0) for _ in range(n)]
    toks = take(len(which))
    halves = [[take(2) for _ in range(4)] for _ in range(2)]
    accs = take(2)
    outs = take(len(which))
    tok_v, w_v, acc_v, h_v, d_v, p_v, sem_t, sem_w, sem_a, sem_d, sem_o = take(11)
    c = core()
    size = [192 if i < 3 else 96 for i in which]
    base = PLACE[which[0]]
    total = sum(size)
    tc, wc, ac, dc = [], [], [], []
    for h in range(2):
        at = spots(c if h == 0 else 1 - c)
        wc.append(
            [
                copy(
                    halves[h][3][j // 2].at[j % 2, :, pl.ds(0, 704)],
                    w_v.at[h, :, :, pl.ds(j * 128, 128)],
                    sem_w.at[h, j],
                )
                for j in range(4)
            ]
        )
        tc.append(
            [
                copy(
                    toks[n].at[:, lanes(at(3, j))],
                    tok_v.at[h, pl.ds(PLACE[i] - base, size[n]), pl.ds(j * 128, 128)],
                    sem_t.at[h, n, j],
                )
                for n, i in enumerate(which)
                for j in range(4)
            ]
        )
        ac.append(copy(accs[h].at[:, pl.ds(base, total)], acc_v.at[h], sem_a.at[h]))
    for h in range(2):
        slot = c if h == 0 else 1 - c
        at = spots(slot)
        for q in range(4):
            for j in range(4):
                for s in range(2):
                    dst = d_v.at[pl.ds(pl.multiple_of(s * 768 + 352 * slot, 16), 352), lanes(at(q, j))]
                    dc.append(copy(halves[h][q][j // 2].at[j % 2, s, pl.ds(704, 352)], dst, sem_d.at[h, q, j, s]))
    for s in range(2):
        d_v[pl.ds(s * 768 + 704, 64), :] = jnp.zeros((64, 2048), BF16)
        h_v[:, pl.ds(s * 768 + 704, 64)] = jnp.zeros((total, 64), BF16)
    for h in range(2):
        for v in wc[h] + tc[h]:
            v.wait()
        ac[h].wait()
        for s in range(2):
            new = product(tok_v[h], w_v[h, s]) + acc_v[h, s]
            if h == 0:
                acc_v[h, s] = new
            else:
                old = acc_v[0, s]
                g, u = jnp.where(c == 0, old, new), jnp.where(c == 0, new, old)
                h_v[:, pl.ds(s * 768, 704)] = (g / (1.0 + jnp.exp(-g)) * u).astype(BF16)
    for v in dc:
        v.wait()
    oc = []
    for n, i in enumerate(which):
        lo = PLACE[i] - base
        for k in range(4):
            cols = pl.ds(k * 512, 512)
            p_v[pl.ds(lo, size[n]), cols] = jnp.dot(
                h_v[pl.ds(lo, size[n])], d_v[:, cols], preferred_element_type=F32
            ).astype(BF16)
        oc.append(copy(p_v.at[pl.ds(lo, size[n])], outs[n], sem_o.at[n]))
    for v in oc:
        v.wait()


def fin(which, tokens, mine, theirs, left, right):
    size = [192 if i < 3 else 96 for i in which]
    total, n = sum(size), len(which)
    operands = [tokens[i] for i in which] + [v for half in (mine, theirs) for pair in half for v in pair] + [left, right]
    scratch = [
        pltpu.VMEM((2, total, 512), BF16),
        pltpu.VMEM((2, 2, 704, 512), BF16),
        pltpu.VMEM((2, 2, total, 704), F32),
        pltpu.VMEM((total, 1536), BF16),
        pltpu.VMEM((1536, 2048), BF16),
        pltpu.VMEM((total, 2048), BF16),
        pltpu.SemaphoreType.DMA((2, n, 4)),
        pltpu.SemaphoreType.DMA((2, 4)),
        pltpu.SemaphoreType.DMA((2,)),
        pltpu.SemaphoreType.DMA((2, 4, 4, 2)),
        pltpu.SemaphoreType.DMA((n,)),
    ]
    shapes = [jax.ShapeDtypeStruct((v, 2048), BF16) for v in size]
    return call(functools.partial(fin_body, which), shapes, operands, scratch, 2 * total * 1408 * (1024 + 2048))


def whole_body(*refs):
    halves, outs, (w_v, sem_w, sem_o) = (refs[:8], refs[8:16]), refs[16:19], refs[19:]
    c = core()
    got = []
    for h in range(2):
        slot = c if h == 0 else 1 - c
        at = spots(slot)
        low = pl.ds(pl.multiple_of(slot * 352, 16), 352)
        for q in range(4):
            for j in range(4):
                src = halves[h][q * 2 + j // 2].at[j % 2, c]
                to = lanes(at(q, j))
                got.append(copy(src.at[pl.ds(0, 704)], w_v.at[slot, :, to], sem_w.at[h, 0, q, j]))
                got.append(copy(src.at[pl.ds(704, 352)], w_v.at[2, low, to], sem_w.at[h, 1, q, j]))
    for v in got:
        v.wait()
    oc = [copy(w_v.at[m], outs[m], sem_o.at[m]) for m in range(3)]
    for v in oc:
        v.wait()


def whole(mine, theirs):
    return call(
        whole_body,
        [jax.ShapeDtypeStruct((704, 2048), BF16)] * 3,
        [v for pair in (*mine, *theirs) for v in pair],
        [pltpu.VMEM((3, 704, 2048), BF16), pltpu.SemaphoreType.DMA((2, 2, 4, 4)), pltpu.SemaphoreType.DMA((3,))],
        2 * 10**9,
    )


def shards(tokens, norm_gain, gate_weight, up_weight, down_weight):
    c = core()
    gain = norm_gain[None, :]
    gate_t = (gate_weight.T * gain).astype(BF16)
    up_t = (up_weight.T * gain).astype(BF16)
    down_t = down_weight.T.astype(BF16)
    a = jnp.concatenate([gate_t, down_t[:352]])
    b = jnp.concatenate([up_t, down_t[352:]])
    keep, give = jnp.where(c == 0, a, b), jnp.where(c == 0, b, a)
    got = swap(give)
    own = jnp.where(c == 0, jnp.stack([keep, got]), jnp.stack([got, keep]))

    before, after, far = send(own, "first", 1), send(own, "first", -1), send(own, "first", 2)
    wide = tokens.astype(F32)
    normed = (wide * lax.rsqrt(jnp.mean(wide * wide, axis=1, keepdims=True) + 1e-06)).astype(BF16)
    left, right = send(normed, "x", 1), send(normed, "x", -1)
    rows = [normed, left, right, send(left[:96], "x", 1), send(right[96:], "x", -1)]
    lo, hi = jnp.stack([own, before]), jnp.stack([after, far])
    lo1, lo2 = send(lo, "second", 1), send(lo, "second", -1)
    hi2, hi1 = send(hi, "second", -1), send(hi, "second", 1)
    mine = [(lo, hi), (lo1, hi1), (lo2, hi2), (send(lo1, "second", 1), send(hi2, "second", -1))]
    theirs = [tuple(swap(v) for v in pair) for pair in mine]

    near = gu(rows, mine, (0, 1, 2), False)
    away = gu(rows, theirs, (0, 1), True)
    away = gu(rows, theirs, (2,), True, away)
    top, bottom = fin((3, 4), rows, mine, theirs, near, away)
    top, bottom = send(top, "x", 1), send(bottom, "x", -1)
    to_left, to_right = fin((1, 2), rows, mine, theirs, near, away)
    add = lambda a, b: (a.astype(F32) + b.astype(F32)).astype(BF16)
    to_right = jnp.concatenate([add(to_right[:96], top), to_right[96:]])
    to_left = jnp.concatenate([to_left[:96], add(to_left[96:], bottom)])
    from_left, from_right = send(to_right, "x", 1), send(to_left, "x", -1)
    (kept,) = fin((0,), rows, mine, theirs, near, away)
    mixed = (kept.astype(F32) + from_left.astype(F32) + from_right.astype(F32)).astype(BF16)
    gate_whole, up_whole, down_whole = whole(mine, theirs)
    return mixed, gate_whole.T, up_whole.T, down_whole.T


def solution(mesh):
    in_specs = (P(("fs", "tp"), None), P("fs"), P("fs", "tp"), P("fs", "tp"), P("fs", "tp"))
    out_specs = (P(("fs", "tp"), None), P(None, "tp"), P(None, "tp"), P(None, "tp"))

    return jax.shard_map(shards, mesh=mesh, in_specs=in_specs, out_specs=out_specs, check_vma=False)
```
